32 devices in a mesh: sp: 4 (over z), fs: 4 (over y, x), tp: 2 (over core).
Axes of the slice: x: 2, y: 2, z: 4, core: 2. Of those that a mesh axis runs over, the one named last changes fastest.
Arguments:
- tokens: bfloat16 [4, 1024, 2048], P('fs', ('sp', 'tp')), may hold values from -6 to 6
- query_weight: bfloat16 [2048, 2048], P(('sp', 'fs'), 'tp'), may hold values from -0.125 to 0.125
- forget_weight: bfloat16 [2048, 2048], P(('sp', 'fs'), 'tp'), may hold values from -0.125 to 0.125
- value_weight: bfloat16 [2048, 2048], P(('sp', 'fs'), 'tp'), may hold values from -0.125 to 0.125
- convolution_gate_weight: bfloat16 [2048, 1024], P(('sp', 'fs'), 'tp'), may hold values from -0.125 to 0.125
- convolution_multiplier_weight: bfloat16 [2048, 1024], P(('sp', 'fs'), 'tp'), may hold values from -0.125 to 0.125
- convolution_input_weight: bfloat16 [2048, 1024], P(('sp', 'fs'), 'tp'), may hold values from -0.125 to 0.125
- gate_headroom: float32 [2048], P('tp'), may hold values from 9.765625e-05 to 0.06
- added_log_rate: float32 [4, 16, 1024], P('fs', 'tp', 'sp'), may hold values from -1.6 to 0
- initial_state: float32 [4, 16, 128, 128], P('fs', 'tp'), may hold values from -0.5 to 0.5
- head_norm_gain: float32 [2048], P('tp'), may hold values from 0.1 to 1.9
- convolution_taps: float32 [3, 1024], P(None, 'tp'), may hold values from -3.5 to 3.5
- convolution_bias: float32 [1024], P('tp'), may hold values from -4 to 4
- recurrence_output_weight: bfloat16 [2048, 2048], P('tp', ('sp', 'fs')), may hold values from -0.109375 to 0.109375
- convolution_output_weight: bfloat16 [1024, 2048], P('tp', ('sp', 'fs')), may hold values from -0.109375 to 0.109375
Outputs:
- mixed: bfloat16 [4, 1024, 2048], P('fs', ('sp', 'tp'))
The draws below stay inside these ranges and needn't reach their ends.
All inputs are finite; a program needn't handle non-finite values.
Results may differ from the reference program's by a relative error of at most 0.018.
Values may be sent and summed in bfloat16 or wider, within the bound.
A program may use at most 64 MiB of HBM per device.

```python
import jax
import jax.numpy as jnp
from jax import lax

D = 2048
RECURRENCE_HEADS = 16
DK = 128
CV = 1024
KW = 3
BLOCK_POSITIONS = 64
TOK = 256
HK = 2048
SEQ = 1024
BATCH = 4
N_TP = 2


def draw_gate_headroom(key, part):
    key_order, key_slow, key_fast = jax.random.split(jax.random.fold_in(key, 11), 3)
    head_order = jax.random.permutation(key_order, RECURRENCE_HEADS)
    slow_count = RECURRENCE_HEADS // 2
    slow_low = 0.25
    slow_high = 1.0
    slow_head = head_order < slow_count
    unit_slow = jax.random.uniform(key_slow, (RECURRENCE_HEADS, DK), jnp.float32)
    unit_fast = jax.random.uniform(key_fast, (RECURRENCE_HEADS, DK), jnp.float32)
    slow_gap = jnp.exp(jnp.log(slow_low) + unit_slow * (jnp.log(slow_high) - jnp.log(slow_low))) / SEQ
    fast_gap = jnp.exp(jnp.log(0.02) + unit_fast * (jnp.log(0.06) - jnp.log(0.02)))
    return jnp.where(slow_head[:, None], slow_gap, fast_gap).reshape(RECURRENCE_HEADS * DK).astype(jnp.float32)


def draw_added_log_rate(key, part):
    key_rate, key_spot, key_kept = jax.random.split(jax.random.fold_in(key, 23), 3)
    span_count = SEQ // TOK
    rate_low = 0.25
    rate_high = 1.0
    block_unit = jax.random.uniform(key_rate, (BATCH, 1, span_count, 1), jnp.float32)
    block_rate = jnp.exp(jnp.log(rate_low) + block_unit * (jnp.log(rate_high) - jnp.log(rate_low))) / SEQ
    stable_part = jnp.broadcast_to(-block_rate, (BATCH, RECURRENCE_HEADS, span_count, TOK)).reshape(BATCH, RECURRENCE_HEADS, SEQ)
    spots = jax.random.randint(key_spot, (BATCH, RECURRENCE_HEADS, 2), 0, SEQ)
    retained_fraction = jax.random.uniform(key_kept, (BATCH, RECURRENCE_HEADS, 2), jnp.float32, minval=0.5, maxval=0.8)
    at_location = jnp.arange(SEQ)[None, None, :, None] == spots[:, :, None, :]
    extra_log_rate = jnp.sum(jnp.where(at_location, jnp.log(retained_fraction)[:, :, None, :], 0.0), axis=-1)
    return (stable_part + extra_log_rate).astype(jnp.float32)


def block_scale(own_key, extent, cuts, low, largest):
    loudness, own = 1.0, jax.random.fold_in(own_key, 6)
    for dim, shards_of in cuts:
        draws = jnp.exp(jax.random.uniform(jax.random.fold_in(own, dim), (shards_of,), jnp.float32, low / len(cuts), largest / len(cuts)))
        loudness = loudness * jnp.repeat(draws, extent[dim] // shards_of).reshape([-1 if axis == dim else 1 for axis in range(len(extent))])
    return loudness


def bell_draw(key, dims, scale, limit, cuts=(), kind=jnp.bfloat16):
    gain = block_scale(key, dims, cuts, -0.22, 0.18) if cuts else 1.0
    entries = jax.random.normal(key, dims, jnp.float32) * scale * gain
    return jnp.minimum(jnp.maximum(entries, -limit), limit).astype(kind)


def setup_inputs(seed: int = 0) -> dict:
    streams_of = jax.random.split(jax.random.key(seed), 16)
    tokens = bell_draw(streams_of[0], (BATCH, SEQ, D), 1.0, 6.0, ((0, 4), (1, 8)))
    query_weight = bell_draw(streams_of[1], (D, HK), D ** -0.5, 0.125, ((0, 16), (1, 2)))
    forget_weight = bell_draw(streams_of[2], (D, HK), D ** -0.5, 0.125, ((0, 16), (1, 2)))
    value_weight = bell_draw(streams_of[3], (D, HK), D ** -0.5, 0.125, ((0, 16), (1, 2)))
    convolution_gate_weight = bell_draw(streams_of[4], (D, CV), D ** -0.5, 0.125, ((0, 16), (1, 2)))
    convolution_multiplier_weight = bell_draw(streams_of[5], (D, CV), D ** -0.5, 0.125, ((0, 16), (1, 2)))
    convolution_input_weight = bell_draw(streams_of[6], (D, CV), D ** -0.5, 0.125, ((0, 16), (1, 2)))
    gate_headroom = draw_gate_headroom(jax.random.fold_in(streams_of[15], 71), 0)
    added_log_rate = draw_added_log_rate(jax.random.fold_in(streams_of[15], 71), 0)
    initial_state = bell_draw(streams_of[9], (BATCH, RECURRENCE_HEADS, DK, DK), (SEQ ** -0.5), 0.5, ((0, 4), (1, 2)), jnp.float32)
    head_norm_gain = jnp.clip(1.0 + 0.18 * jax.random.normal(streams_of[10], (HK,), jnp.float32), 0.1, 1.9)
    convolution_taps = bell_draw(streams_of[11], (KW, CV), KW ** -0.5, 3.5, ((1, 2),), jnp.float32)
    convolution_bias = bell_draw(streams_of[12], (CV,), 1.0, 4.0, ((0, 2),), jnp.float32)
    recurrence_output_weight = bell_draw(streams_of[13], (HK, D), (HK + CV) ** -0.5, 0.109375, ((0, 2), (1, 16)))
    convolution_output_weight = bell_draw(streams_of[14], (CV, D), (HK + CV) ** -0.5, 0.109375, ((0, 2), (1, 16)))
    return {"tokens": tokens, "query_weight": query_weight, "forget_weight": forget_weight, "value_weight": value_weight, "convolution_gate_weight": convolution_gate_weight, "convolution_multiplier_weight": convolution_multiplier_weight, "convolution_input_weight": convolution_input_weight, "gate_headroom": gate_headroom, "added_log_rate": added_log_rate, "initial_state": initial_state, "head_norm_gain": head_norm_gain, "convolution_taps": convolution_taps, "convolution_bias": convolution_bias, "recurrence_output_weight": recurrence_output_weight, "convolution_output_weight": convolution_output_weight}


def project(sequence_rows, weight):
    return jnp.dot(sequence_rows, weight, preferred_element_type=jnp.float32).astype(jnp.bfloat16)

def to_blocks(values, number_of_blocks):
    return jnp.transpose(values.reshape(number_of_blocks, BLOCK_POSITIONS, RECURRENCE_HEADS, DK), (2, 0, 1, 3))

def gated_recurrence(query_vectors, forget_logits, value_vectors, gate_headroom, extra_rates, opening_state):
    length = query_vectors.shape[0]
    number_of_blocks = length // BLOCK_POSITIONS
    query_scaled = to_blocks(query_vectors.astype(jnp.float32), number_of_blocks) * DK ** (-0.5)
    gated_key = to_blocks(gate_headroom[None, :] * jax.nn.sigmoid(-forget_logits.astype(jnp.float32)), number_of_blocks)
    forget_log_rate = jnp.log1p(-gated_key) + extra_rates.reshape(RECURRENCE_HEADS, number_of_blocks, BLOCK_POSITIONS)[..., None]
    values = to_blocks(value_vectors.astype(jnp.float32), number_of_blocks)
    cumulative = jnp.cumsum(forget_log_rate, axis=2)
    query_decayed = query_scaled * jnp.exp(cumulative)
    key_decayed = gated_key * jnp.exp(-cumulative)
    scores = jnp.einsum('hnik,hnjk->hnij', query_decayed, key_decayed, precision=lax.Precision.HIGHEST)
    causal = jnp.tril(jnp.ones((BLOCK_POSITIONS, BLOCK_POSITIONS), dtype=bool))
    scores = jnp.where(causal, scores, 0.0)
    within = jnp.einsum('hnij,hnjv->hniv', scores, values, precision=lax.Precision.HIGHEST)
    final_log = cumulative[:, :, -1:, :]
    contrib = jnp.einsum('hnck,hncv->hnkv', gated_key * jnp.exp(final_log - cumulative), values, precision=lax.Precision.HIGHEST)
    decays = jnp.exp(final_log[:, :, 0, :])

    def advance(current, block_pair):
        return (block_pair[0][..., None] * current + block_pair[1], current)
    _, entering = lax.scan(advance, opening_state, (jnp.moveaxis(decays, 1, 0), jnp.moveaxis(contrib, 1, 0)))
    entering = jnp.moveaxis(entering, 0, 1)
    carried_term = jnp.einsum('hnck,hnkv->hncv', query_decayed, entering, precision=lax.Precision.HIGHEST)
    return jnp.transpose(within + carried_term, (1, 2, 0, 3)).reshape(length, RECURRENCE_HEADS, DK)

def reference(tokens, query_weight, forget_weight, value_weight, convolution_gate_weight, convolution_multiplier_weight, convolution_input_weight, gate_headroom, added_log_rate, initial_state, head_norm_gain, convolution_taps, convolution_bias, recurrence_output_weight, convolution_output_weight):

    def single_sequence(input_rows):
        sequence_rows, extra_rates, opening_state = input_rows
        length = sequence_rows.shape[0]
        query_vectors = project(sequence_rows, query_weight)
        forget_logits = project(sequence_rows, forget_weight)
        value_vectors = project(sequence_rows, value_weight)
        conv_gate = project(sequence_rows, convolution_gate_weight)
        conv_mult = project(sequence_rows, convolution_multiplier_weight)
        conv_input = project(sequence_rows, convolution_input_weight)
        recurrence_unnormed = gated_recurrence(query_vectors, forget_logits, value_vectors, gate_headroom, extra_rates, opening_state)
        mean_square = lax.optimization_barrier(jnp.mean(recurrence_unnormed * recurrence_unnormed, axis=-1, keepdims=True))
        rec_out = recurrence_unnormed * lax.rsqrt(mean_square + 1e-06) * head_norm_gain.reshape(RECURRENCE_HEADS, DK)
        rec_out = rec_out.reshape(length, HK).astype(jnp.bfloat16)
        conv_prod = conv_mult.astype(jnp.float32) * conv_input.astype(jnp.float32)
        padded = jnp.concatenate([jnp.zeros((KW - 1, CV), jnp.float32), conv_prod], axis=0)
        conv_y = jnp.broadcast_to(convolution_bias[None, :], (length, CV))
        for j in range(KW):
            conv_y = conv_y + convolution_taps[j][None, :] * padded[j:j + length]
        conv_out = (conv_gate.astype(jnp.float32) * conv_y).astype(jnp.bfloat16)
        rec_group = HK // N_TP
        conv_group = CV // N_TP
        running = jnp.zeros((length, D), jnp.float32)
        for g in range(N_TP):
            partial_value = jnp.dot(rec_out[:, g * rec_group:(g + 1) * rec_group], recurrence_output_weight[g * rec_group:(g + 1) * rec_group], preferred_element_type=jnp.float32)
            partial_value = partial_value + jnp.dot(conv_out[:, g * conv_group:(g + 1) * conv_group], convolution_output_weight[g * conv_group:(g + 1) * conv_group], preferred_element_type=jnp.float32)
            running = running + lax.optimization_barrier(partial_value.astype(jnp.bfloat16)).astype(jnp.float32)
        return running.astype(jnp.bfloat16)
    return lax.map(single_sequence, (tokens, added_log_rate, initial_state))
```

```python
import functools

import jax
import jax.numpy as jnp
from jax import lax
from jax.experimental import pallas as pl
from jax.experimental.pallas import tpu as pltpu
from jax.sharding import PartitionSpec as P

DK = 128
KW = 3
BLOCK_POSITIONS = 64


def carried_in(part, axis, combine, identity):
    place = lax.axis_index(axis)
    gathered = jax.tree.map(lambda a: lax.all_gather(a, axis), part)
    state = jax.tree.map(lambda a, e: jnp.zeros_like(a) + jnp.asarray(e, a.dtype), part, identity)

    def one(hop, state):
        return combine(
            state, jax.tree.map(lambda a: lax.dynamic_index_in_dim(a, hop, 0, False), gathered)
        )

    return lax.fori_loop(0, place, one, state)


def from_behind(block, axis, distance):
    devices = range(lax.axis_size(axis))
    route = [(i - distance, i) for i in devices if i - distance in devices]
    return lax.ppermute(block, axis, route)


def to_blocks(values, number_of_heads):
    number_of_blocks = values.shape[0] // BLOCK_POSITIONS
    return jnp.transpose(
        values.reshape(number_of_blocks, BLOCK_POSITIONS, number_of_heads, DK), (2, 0, 1, 3)
    )


def within_block_recurrence(
    query_vectors, forget_logits, value_vectors, gate_headroom, extra_rates
):
    number_of_heads = extra_rates.shape[0]
    number_of_blocks = query_vectors.shape[0] // BLOCK_POSITIONS
    query_scaled = to_blocks(query_vectors.astype(jnp.float32), number_of_heads) * DK ** (-0.5)
    gated_key = to_blocks(
        gate_headroom[None, :] * jax.nn.sigmoid(-forget_logits.astype(jnp.float32)), number_of_heads
    )
    forget_log_rate = (
        jnp.log1p(-gated_key)
        + extra_rates.reshape(number_of_heads, number_of_blocks, BLOCK_POSITIONS)[..., None]
    )
    values = to_blocks(value_vectors.astype(jnp.float32), number_of_heads)
    cumulative = jnp.cumsum(forget_log_rate, axis=2)
    query_decayed = query_scaled * jnp.exp(cumulative)
    key_decayed = gated_key * jnp.exp(-cumulative)
    scores = jnp.einsum(
        "hnik,hnjk->hnij", query_decayed, key_decayed, precision=lax.Precision.HIGHEST
    )
    causal = jnp.tril(jnp.ones((BLOCK_POSITIONS, BLOCK_POSITIONS), dtype=bool))
    scores = jnp.where(causal, scores, 0.0)
    within = jnp.einsum("hnij,hnjv->hniv", scores, values, precision=lax.Precision.HIGHEST)
    final_log = cumulative[:, :, -1, :]
    contrib = jnp.einsum(
        "hnck,hncv->hnkv",
        gated_key * jnp.exp(final_log[:, :, None, :] - cumulative),
        values,
        precision=lax.Precision.HIGHEST,
    )
    decays = jnp.exp(final_log)

    def advance(current, block_pair):
        return (block_pair[0][..., None] * current + block_pair[1], current)

    empty_state = jnp.zeros((number_of_heads, DK, DK), jnp.float32)
    local_total, entering = lax.scan(
        advance, empty_state, (jnp.moveaxis(decays, 1, 0), jnp.moveaxis(contrib, 1, 0))
    )
    entering = jnp.moveaxis(entering, 0, 1)
    before = jnp.exp(jnp.cumsum(final_log, axis=1) - final_log)
    device_decay = jnp.exp(jnp.sum(final_log, axis=1))
    return (query_decayed, within, entering, before, device_decay, local_total)


def finish(query_decayed, within, entering, before, carried, head_norm_gain):
    number_of_heads = query_decayed.shape[0]
    states = entering + before[..., None] * carried[:, None]
    carried_term = jnp.einsum(
        "hnck,hnkv->hncv", query_decayed, states, precision=lax.Precision.HIGHEST
    )
    length = query_decayed.shape[1] * BLOCK_POSITIONS
    recurrence_unnormed = jnp.transpose(within + carried_term, (1, 2, 0, 3)).reshape(
        length, number_of_heads, DK
    )
    mean_square = jnp.mean(recurrence_unnormed * recurrence_unnormed, axis=-1, keepdims=True)
    rec_out = (
        recurrence_unnormed
        * lax.rsqrt(mean_square + 1e-06)
        * head_norm_gain.reshape(number_of_heads, DK)
    )
    return rec_out.reshape(length, number_of_heads * DK).astype(jnp.bfloat16)


def chain_combine(earlier_part, later_part):
    return (
        earlier_part[0] * later_part[0],
        later_part[0][..., None] * earlier_part[1] + later_part[1],
    )


def shards(
    tokens,
    query_weight,
    forget_weight,
    value_weight,
    convolution_gate_weight,
    convolution_multiplier_weight,
    convolution_input_weight,
    gate_headroom,
    added_log_rate,
    initial_state,
    head_norm_gain,
    convolution_taps,
    convolution_bias,
    recurrence_output_weight,
    convolution_output_weight,
):
    own_rows = tokens[0]
    gathered = (
        lax.all_gather(query_weight, ("sp", "fs"), axis=0, tiled=True),
        lax.all_gather(forget_weight, ("sp", "fs"), axis=0, tiled=True),
        lax.all_gather(value_weight, ("sp", "fs"), axis=0, tiled=True),
        lax.all_gather(convolution_gate_weight, ("sp", "fs"), axis=0, tiled=True),
        lax.all_gather(convolution_multiplier_weight, ("sp", "fs"), axis=0, tiled=True),
        lax.all_gather(convolution_input_weight, ("sp", "fs"), axis=0, tiled=True),
        lax.all_gather(recurrence_output_weight, ("sp", "fs"), axis=1, tiled=True),
        lax.all_gather(convolution_output_weight, ("sp", "fs"), axis=1, tiled=True),
    )
    in_weights = gathered[:6]
    out_rec = gathered[6]
    out_conv = gathered[7]
    block_rows = lax.all_gather(own_rows, "tp", axis=0, tiled=True)
    projected = jnp.concatenate(
        [
            jnp.dot(block_rows, weight, preferred_element_type=jnp.float32).astype(jnp.bfloat16)
            for weight in in_weights
        ],
        axis=1,
    )
    rec_width = query_weight.shape[1]
    conv_width = convolution_gate_weight.shape[1]
    query_vectors = projected[:, :rec_width]
    forget_logits = projected[:, rec_width : 2 * rec_width]
    value_vectors = projected[:, 2 * rec_width : 3 * rec_width]
    conv_base = 3 * rec_width
    conv_gate = projected[:, conv_base : conv_base + conv_width]
    conv_mult = projected[:, conv_base + conv_width : conv_base + 2 * conv_width]
    conv_input = projected[:, conv_base + 2 * conv_width : conv_base + 3 * conv_width]
    query_decayed, within, entering, before, device_decay, local_total = within_block_recurrence(
        query_vectors, forget_logits, value_vectors, gate_headroom, added_log_rate[0]
    )
    conv_prod = conv_mult.astype(jnp.float32) * conv_input.astype(jnp.float32)
    length = conv_prod.shape[0]
    tail_rows = conv_prod[length - (KW - 1) :]
    unit_decay = jnp.ones_like(device_decay)
    empty_state = jnp.zeros_like(local_total)
    prior_decay, prior_state = carried_in(
        (device_decay, local_total), "sp", chain_combine, (unit_decay, empty_state)
    )
    prior_rows = from_behind(tail_rows, "sp", 1)
    carried = prior_decay[..., None] * initial_state[0] + prior_state
    rec_out = finish(query_decayed, within, entering, before, carried, head_norm_gain)
    extended = jnp.concatenate([prior_rows, conv_prod], axis=0)
    conv_y = jnp.broadcast_to(convolution_bias[None, :], conv_prod.shape)
    for j in range(KW):
        conv_y = conv_y + convolution_taps[j][None, :] * extended[j : j + length]
    conv_out = (conv_gate.astype(jnp.float32) * conv_y).astype(jnp.bfloat16)
    mixed = lax.psum_scatter(
        (
            jnp.dot(rec_out, out_rec, preferred_element_type=jnp.float32)
            + jnp.dot(conv_out, out_conv, preferred_element_type=jnp.float32)
        ).astype(jnp.bfloat16),
        "tp",
        scatter_dimension=0,
        tiled=True,
    )
    return mixed[None]


MESH = pl.DeviceIdType.MESH
F32 = jnp.float32
BF16 = jnp.bfloat16
CONTRACT_LAST = (((1,), (1,)), ((), ()))
CONTRACT_FIRST = (((0,), (0,)), ((), ()))


def layer_kernel(
    n_sp, n_fs, tok, wq, wf, wv, cg, cm, ci, ro, co, headroom, rate, init, gain, taps, bias,
    out, tokens, win, wout, rates, state, ext, sib_send, sib_recv, mine, z_send, z_recv,
    loc_sem, send_sem, win_z, wout_z, win_f, wout_f, tok_z, tok_t, rate_z, sib_sem, zr_sem,
    rs_send,
):
    sp, fs, tp = lax.axis_index("sp"), lax.axis_index("fs"), lax.axis_index("tp")
    other = 1 - tp
    rows = wq.shape[0]
    rec = wq.shape[1] // n_sp
    con = cg.shape[1] // n_sp
    span = tok.shape[0]
    heads = rec // DK
    wide = tok.shape[1]

    def peer(**where):
        return {"sp": where.get("sp", sp), "fs": where.get("fs", fs), "tp": where.get("tp", tp)}

    def z_at(d):
        return lax.rem(sp + d, n_sp)

    def f_at(e):
        return lax.rem(fs + e, n_fs)

    parts = []
    at = 0
    for ref, width in ((wq, rec), (wf, rec), (wv, rec), (cg, con), (cm, con), (ci, con)):
        parts.append((ref, at, width))
        at += width

    def in_slot(s, f):
        return win.at[pl.ds(pl.multiple_of((s * n_fs + f) * rows, rows), rows)]

    def in_piece(s, f, at, width):
        first = pl.multiple_of((s * n_fs + f) * rows, rows)
        return win.at[pl.ds(first, rows), pl.ds(at, width)]

    def out_slot(s, f):
        lanes = ro.shape[1]
        return wout.at[:, pl.ds(pl.multiple_of((s * n_fs + f) * lanes, lanes), lanes)]

    def out_piece(s, f, at, width):
        lanes = ro.shape[1]
        first = pl.multiple_of((s * n_fs + f) * lanes, lanes)
        return wout.at[pl.ds(at, width), pl.ds(first, lanes)]

    def weight_sources(s):
        ins = [
            (ref.at[:, pl.ds(pl.multiple_of(s * width, width), width)], at, width)
            for ref, at, width in parts
        ]
        outs = [
            (ro.at[pl.ds(pl.multiple_of(s * rec, rec), rec)], 0, rec),
            (co.at[pl.ds(pl.multiple_of(s * con, con), con)], rec, con),
        ]
        return ins, outs

    local = []
    ins, outs = weight_sources(sp)
    for ref, at, width in ins:
        local.append((ref, in_piece(sp, fs, at, width)))
    for ref, at, width in outs:
        local.append((ref, out_piece(sp, fs, at, width)))
    local.append((tok, tokens.at[sp * 2 + tp]))
    local.append((rate.at[sp], rates.at[sp]))
    local = [pltpu.make_async_copy(*pair, loc_sem.at[i]) for i, pair in enumerate(local)]
    for copy in local:
        copy.start()

    barrier = pltpu.get_barrier_semaphore()
    for d in range(1, n_sp):
        pl.semaphore_signal(barrier, inc=1, device_id=peer(sp=z_at(d)), device_id_type=MESH)
    for e in range(1, n_fs):
        pl.semaphore_signal(barrier, inc=1, device_id=peer(fs=f_at(e)), device_id_type=MESH)
    pl.semaphore_signal(barrier, inc=1, device_id=peer(tp=other), device_id_type=MESH)
    pl.semaphore_wait(barrier, n_sp + n_fs - 1)

    sent = []

    def remote(src, dst, recv, to, start=True):
        copy = pltpu.make_async_remote_copy(
            src_ref=src, dst_ref=dst, send_sem=send_sem.at[len(sent) if start else 0], recv_sem=recv, device_id=to,
            device_id_type=MESH,
        )
        if start:
            copy.start()
            sent.append(copy)
        return copy

    near = sorted(range(1, n_sp), key=lambda d: min(d, n_sp - d))
    for d in near:
        to = peer(sp=z_at(d))
        ins, outs = weight_sources(z_at(d))
        for i, (ref, at, width) in enumerate(ins):
            remote(ref, in_piece(sp, fs, at, width), win_z.at[d, i], to)
        for i, (ref, at, width) in enumerate(outs):
            remote(ref, out_piece(sp, fs, at, width), wout_z.at[d, i], to)
        remote(tok, tokens.at[sp * 2 + tp], tok_z.at[d], to)
        remote(rate.at[z_at(d)], rates.at[sp], rate_z.at[d], to)
    remote(tok, tokens.at[sp * 2 + tp], tok_t.at[0], peer(tp=other))

    for copy in local:
        copy.wait()

    def spread(d):
        s = z_at(n_sp - d)
        for e in range(1, n_fs):
            remote(in_slot(s, fs), in_slot(s, fs), win_f.at[e, d], peer(fs=f_at(e)))
        for e in range(1, n_fs):
            remote(out_slot(s, fs), out_slot(s, fs), wout_f.at[e, d], peer(fs=f_at(e)))

    spread(0)
    for d in near:
        s = z_at(n_sp - d)
        me = peer(tp=other)
        for i, (ref, at, width) in enumerate(parts):
            piece = in_piece(s, fs, at, width)
            remote(piece, piece, win_z.at[d, i], me, start=False).wait_recv()
        for i, (at, width) in enumerate(((0, rec), (rec, con))):
            piece = out_piece(s, fs, at, width)
            remote(piece, piece, wout_z.at[d, i], me, start=False).wait_recv()
        spread(d)
        piece = tokens.at[s * 2 + tp]
        remote(piece, piece, tok_z.at[d], me, start=False).wait_recv()
        remote(piece, piece, tok_t.at[d], me)
        remote(rates.at[s], rates.at[s], rate_z.at[d], me, start=False).wait_recv()
    for d in range(n_sp):
        s = z_at((n_sp - d) % n_sp)
        piece = tokens.at[s * 2 + other]
        remote(piece, piece, tok_t.at[d], peer(tp=other), start=False).wait_recv()
    for d in range(n_sp):
        s = z_at((n_sp - d) % n_sp)
        for e in range(1, n_fs):
            f = f_at(n_fs - e)
            remote(in_slot(s, f), in_slot(s, f), win_f.at[e, d], peer(tp=other), start=False).wait_recv()
            remote(out_slot(s, f), out_slot(s, f), wout_f.at[e, d], peer(tp=other), start=False).wait_recv()
    for copy in sent:
        copy.wait_send()

    for h in range(heads):
        state[h] = init[sp * heads + h].T
    ext[0:8] = jnp.zeros((8, con), F32)
    lane_rec = pl.ds(pl.multiple_of(sp * rec, rec), rec)
    lane_con = pl.ds(pl.multiple_of(sp * con, con), con)
    row_id = lax.broadcasted_iota(jnp.int32, (span, span), 0)
    col_id = lax.broadcasted_iota(jnp.int32, (span, span), 1)
    causal = row_id >= col_id
    lower = causal.astype(F32)
    upper = (row_id <= col_id).astype(F32)
    length = 2 * span

    def sib_copy(s):
        return pltpu.make_async_remote_copy(
            src_ref=sib_send.at[s], dst_ref=sib_recv.at[s], send_sem=rs_send.at[0, s],
            recv_sem=sib_sem.at[s], device_id=peer(tp=other), device_id_type=MESH,
        )

    def z_copy(s):
        d = lax.rem(s - sp + n_sp, n_sp)
        return pltpu.make_async_remote_copy(
            src_ref=z_send.at[s], dst_ref=z_recv.at[d], send_sem=rs_send.at[1, d],
            recv_sem=zr_sem.at[d], device_id=peer(sp=s), device_id_type=MESH,
        )

    def pass_on(s):
        sib_copy(s).wait_recv()
        total = mine[s] + sib_recv[s].astype(F32)

        @pl.when(s != sp)
        def _():
            z_send[s] = total.astype(BF16)
            z_copy(s).start()

        @pl.when(s == sp)
        def _():
            z_recv[0] = total.astype(BF16)

    def step(s, carry):
        block = jnp.concatenate([tokens[2 * s], tokens[2 * s + 1]], axis=0)

        def project(at, width):
            return jnp.dot(
                block, win[:, pl.ds(at, width)], preferred_element_type=F32
            ).astype(BF16)

        query = project(0, rec).astype(F32) * DK ** (-0.5)
        forget = project(rec, rec).astype(F32)
        value = project(2 * rec, rec)
        base = 3 * rec
        conv_gate = project(base, con).astype(F32)
        prod = project(base + con, con).astype(F32) * project(base + 2 * con, con).astype(F32)
        key_gate = headroom[:, lane_rec] * jax.nn.sigmoid(-forget)
        log_forget = jnp.log1p(-key_gate)
        gains = gain[:, lane_rec]
        halves = []
        for c in range(2):
            part = slice(c * span, (c + 1) * span)
            cum = jnp.dot(lower, log_forget[part], precision=lax.Precision.HIGHEST)
            extra = jnp.dot(rates[s][:, part], upper, precision=lax.Precision.HIGHEST)
            extra_t = extra.T
            grow = jnp.exp(cum)
            query_grow = query[part] * grow
            key_grow = (key_gate[part] / grow).astype(BF16)
            last = cum[span - 1 :, :]
            key_last = key_gate[part] * jnp.exp(last - cum)
            last_decay = jnp.exp(last)
            pieces = []
            for h in range(heads):
                lanes = slice(h * DK, (h + 1) * DK)
                row = extra[h : h + 1]
                column = extra_t[:, h : h + 1]
                end = row[:, span - 1 :]
                scores = lax.dot_general(
                    query_grow[:, lanes].astype(BF16), key_grow[:, lanes], CONTRACT_LAST,
                    preferred_element_type=F32,
                )
                decay = jnp.exp(jnp.where(causal, column - row, 0.0))
                scores = jnp.where(causal, scores * decay, 0.0).astype(BF16)
                values = value[part, lanes]
                before = state[h]
                raw = jnp.dot(scores, values, preferred_element_type=F32)
                raw = raw + lax.dot_general(
                    (query_grow[:, lanes] * jnp.exp(column)).astype(BF16), before.astype(BF16),
                    CONTRACT_LAST, preferred_element_type=F32,
                )
                keys = (key_last[:, lanes] * jnp.exp(end - column)).astype(BF16)
                state[h] = before * (last_decay[:, lanes] * jnp.exp(end)) + lax.dot_general(
                    values, keys, CONTRACT_FIRST, preferred_element_type=F32
                )
                square = jnp.mean(raw * raw, axis=-1, keepdims=True)
                pieces.append((raw * lax.rsqrt(square + 1e-06) * gains[:, lanes]).astype(BF16))
            halves.append(jnp.concatenate(pieces, axis=1))
        ext[8:] = prod
        conv = jnp.broadcast_to(bias[:, lane_con], prod.shape)
        for j in range(KW):
            conv = conv + taps[j : j + 1, lane_con] * ext[pl.ds(8 - (KW - 1) + j, length)]
        ext[0:8] = ext[length:]
        conv_out = (conv_gate * conv).astype(BF16)
        both = jnp.concatenate([jnp.concatenate(halves, axis=0), conv_out], axis=1)
        chunk = min(512, wide)
        for n in range(0, wide, chunk):
            partial = jnp.dot(both, wout[:, n : n + chunk], preferred_element_type=F32)
            first = partial[:span]
            second = partial[span:]
            mine[s, :, n : n + chunk] = jnp.where(tp == 0, first, second)
            sib_send[s, :, n : n + chunk] = jnp.where(tp == 0, second, first).astype(BF16)
        sib_copy(s).start()

        @pl.when(s > 0)
        def _():
            pass_on(s - 1)

        return carry

    lax.fori_loop(0, n_sp, step, 0)
    pass_on(n_sp - 1)
    for d in range(1, n_sp):
        pltpu.make_async_remote_copy(
            src_ref=z_recv.at[d], dst_ref=z_recv.at[d], send_sem=rs_send.at[1, d],
            recv_sem=zr_sem.at[d], device_id=peer(tp=other), device_id_type=MESH,
        ).wait_recv()
    total = z_recv[0].astype(F32)
    for d in range(1, n_sp):
        total = total + z_recv[d].astype(F32)
    out[...] = total.astype(BF16)
    for s in range(n_sp):
        sib_copy(s).wait_send()
    for d in range(1, n_sp):
        pltpu.make_async_remote_copy(
            src_ref=z_send.at[z_at(d)], dst_ref=z_recv.at[d], send_sem=rs_send.at[1, d],
            recv_sem=zr_sem.at[d], device_id=peer(sp=z_at(d)), device_id_type=MESH,
        ).wait_send()


def sequence_shards(n_sp, n_fs, *arrays):
    (tok, wq, wf, wv, cg, cm, ci, headroom, rate, init, gain, taps, bias, ro, co) = arrays
    span, wide = tok.shape[1:]
    rec, con = wq.shape[1] // n_sp, cg.shape[1] // n_sp
    heads = rec // DK
    by_place = rate[0].reshape(n_sp, heads, rate.shape[2])
    by_place = jnp.pad(by_place, ((0, 0), (0, 8 - heads), (0, 0)))
    hbm = pl.BlockSpec(memory_space=pl.ANY)
    vmem = pl.BlockSpec(memory_space=pltpu.VMEM)
    dma = pltpu.SemaphoreType.DMA
    mixed = pl.pallas_call(
        functools.partial(layer_kernel, n_sp, n_fs),
        out_shape=jax.ShapeDtypeStruct((span, wide), BF16),
        in_specs=[hbm] * 9 + [vmem, hbm] + [vmem] * 4,
        out_specs=vmem,
        scratch_shapes=[
            pltpu.VMEM((2 * n_sp, span, wide), BF16),
            pltpu.VMEM((wide, 3 * (rec + con)), BF16),
            pltpu.VMEM((rec + con, wide), BF16),
            pltpu.VMEM((n_sp, 8, rate.shape[2]), F32),
            pltpu.VMEM((heads, DK, DK), F32),
            pltpu.VMEM((8 + 2 * span, con), F32),
            pltpu.VMEM((n_sp, span, wide), BF16),
            pltpu.VMEM((n_sp, span, wide), BF16),
            pltpu.VMEM((n_sp, span, wide), F32),
            pltpu.VMEM((n_sp, span, wide), BF16),
            pltpu.VMEM((n_sp, span, wide), BF16),
            dma((10,)),
            dma(((n_sp - 1) * 10 + n_sp * (1 + 2 * (n_fs - 1)),)),
            dma((n_sp, 6)),
            dma((n_sp, 2)),
            dma((n_fs, n_sp)),
            dma((n_fs, n_sp)),
            dma((n_sp,)),
            dma((n_sp,)),
            dma((n_sp,)),
            dma((n_sp,)),
            dma((n_sp,)),
            dma((2, n_sp)),
        ],
        compiler_params=pltpu.CompilerParams(
            collective_id=0, has_side_effects=True, vmem_limit_bytes=60 * 2**20
        ),
    )(
        tok[0], wq, wf, wv, cg, cm, ci, ro, co, headroom[None], by_place, init[0], gain[None],
        taps, bias[None],
    )
    return mixed[None]


def choose_plan(sizes, *arrays):
    n_sp, n_fs = sizes["sp"], sizes["fs"]
    rows, rec = arrays[1].shape
    con = arrays[4].shape[1]
    span = arrays[0].shape[1]
    even = (
        sizes["tp"] == 2
        and arrays[0].shape[0] == 1
        and rec % (n_sp * DK) == 0
        and rec // (n_sp * DK) <= 8
        and con % (n_sp * 128) == 0
        and rows % 128 == 0
        and span == DK
        and arrays[13].shape[1] % 128 == 0
    )
    return sequence_shards(n_sp, n_fs, *arrays) if even else shards(*arrays)


def solution(mesh):
    in_specs = (
        P("fs", ("sp", "tp"), None),
        P(("sp", "fs"), "tp"),
        P(("sp", "fs"), "tp"),
        P(("sp", "fs"), "tp"),
        P(("sp", "fs"), "tp"),
        P(("sp", "fs"), "tp"),
        P(("sp", "fs"), "tp"),
        P("tp"),
        P("fs", "tp", "sp"),
        P("fs", "tp", None, None),
        P("tp"),
        P(None, "tp"),
        P("tp"),
        P("tp", ("sp", "fs")),
        P("tp", ("sp", "fs")),
    )
    out_specs = P("fs", ("sp", "tp"), None)
    body = functools.partial(choose_plan, dict(mesh.shape))
    return jax.shard_map(body, mesh=mesh, in_specs=in_specs, out_specs=out_specs, check_vma=False)
```
